32 devices in a mesh: tp: 8 (over z, x), dp: 4 (over y, core).
Axes of the slice: x: 2, y: 2, z: 4, core: 2. Of those that a mesh axis runs over, the one named last changes fastest.
Arguments:
- tokens: bfloat16 [64, 4096], P('dp', 'tp'), may hold values from -6 to 6
- norm_gain: float32 [2, 4096], replicated, may hold values from 0.1 to 1.9
- w_in: bfloat16 [2, 4096, 2048], P(None, 'dp', 'tp'), may hold values from -0.09375 to 0.09375
- w_gate: bfloat16 [2, 4096, 2048], P(None, 'dp', 'tp'), may hold values from -0.1875 to 0.1875
- decay_rate: float32 [2, 128, 64], P(None, 'tp'), may hold values from 0.05 to 2
- frequency: float32 [2, 128, 64], P(None, 'tp'), may hold values from -3 to 3
- log_step: float32 [2, 128], P(None, 'tp'), may hold values from -3 to 0
- map_re: float32 [2, 128, 16, 64], P(None, 'tp'), may hold values from -1.5 to 1.5
- map_im: float32 [2, 128, 16, 64], P(None, 'tp'), may hold values from -1.5 to 1.5
- read_re: float32 [2, 128, 16, 64], P(None, 'tp'), may hold values from -0.5 to 0.5
- read_im: float32 [2, 128, 16, 64], P(None, 'tp'), may hold values from -0.5 to 0.5
- skip_weight: float32 [2, 128, 16], P(None, 'tp'), may hold values from -4 to 4
- w_out: bfloat16 [2, 2048, 4096], P(None, 'dp', 'tp'), may hold values from -0.25 to 0.25
- state_re: float32 [2, 64, 128, 64], P(None, 'dp', 'tp'), may hold values from -6 to 6
- state_im: float32 [2, 64, 128, 64], P(None, 'dp', 'tp'), may hold values from -6 to 6
Outputs:
- hidden: bfloat16 [64, 4096], P('dp', 'tp')
- new_re: float32 [2, 64, 128, 64], P(None, 'dp', 'tp')
- new_im: float32 [2, 64, 128, 64], P(None, 'dp', 'tp')
The draws below stay inside these ranges and needn't reach their ends.
All inputs are finite; a program needn't handle non-finite values.
Results may differ from the reference program's by a relative error of at most 0.01.
Values may be sent and summed in bfloat16 or wider, within the bound.
A program may use at most 64 MiB of HBM per device.

```python
import math
import jax
import jax.numpy as jnp
from jax import lax

D = 4096
GROUPS = 128
GROUP_CH = 16
STATE_N = 64
LAYERS = 2
WIDTH = 2048
SEQS = 64


def block_scale(rng, extent, cuts, smallest, high):
    def one(position, blocks):
        heights = jax.random.uniform(jax.random.fold_in(jax.random.fold_in(rng, 6), position), (blocks,), jnp.float32, smallest / len(cuts), high / len(cuts))
        return jnp.repeat(jnp.exp(heights), extent[position] // blocks).reshape((-1,) + (1,) * (len(extent) - position - 1))

    loudness = one(*cuts[0])
    for cut in cuts[1:]:
        loudness = loudness * one(*cut)
    return loudness


def normal_values(own_key, extent, deviation, reach, shards=(), dtype=jnp.bfloat16):
    result = deviation * jax.random.normal(own_key, extent, jnp.float32)
    if shards:
        result = result * block_scale(own_key, extent, shards, -0.22, 0.18)
    return jnp.clip(result, -reach, reach).astype(dtype)


def setup_inputs(seed: int = 0) -> dict:
    streams_of = jax.random.split(jax.random.key(seed), 16)
    return {
        "tokens": normal_values(streams_of[0], (SEQS, D), 1.0, 6.0, ((0, 4), (1, 8))),
        "norm_gain": jnp.clip(1.0 + 0.18 * jax.random.normal(streams_of[1], (LAYERS, D), jnp.float32), 0.1, 1.9),
        "w_in": normal_values(streams_of[2], (LAYERS, D, WIDTH), D ** -0.5, 0.09375, ((1, 4), (2, 8))),
        "w_gate": normal_values(streams_of[3], (LAYERS, D, WIDTH), (D // 4) ** -0.5, 0.1875, ((1, 4), (2, 8))),
        "decay_rate": jnp.clip(jnp.exp(math.log(2.0) - 3.6888794 * jax.random.uniform(streams_of[4], (LAYERS, GROUPS, STATE_N), jnp.float32) ** block_scale(streams_of[4], (LAYERS, GROUPS, STATE_N), ((1, 8),), -0.2, 0.2)), 0.05, 2.0),
        "frequency": jnp.clip(jax.random.uniform(streams_of[5], (LAYERS, GROUPS, STATE_N), jnp.float32, -3.0, 3.0) * block_scale(streams_of[5], (LAYERS, GROUPS, STATE_N), ((1, 8),), -0.4, 0.0), -3.0, 3.0),
        "log_step": jnp.clip(-3.0 + 3.0 * jax.random.uniform(streams_of[6], (LAYERS, GROUPS), jnp.float32) ** block_scale(streams_of[6], (LAYERS, GROUPS), ((1, 8),), -0.2, 0.2), -3.0, 0.0),
        "map_re": normal_values(streams_of[7], (LAYERS, GROUPS, GROUP_CH, STATE_N), GROUP_CH ** -0.5, 1.5, ((1, 8),), jnp.float32),
        "map_im": normal_values(streams_of[8], (LAYERS, GROUPS, GROUP_CH, STATE_N), GROUP_CH ** -0.5, 1.5, ((1, 8),), jnp.float32),
        "read_re": normal_values(streams_of[9], (LAYERS, GROUPS, GROUP_CH, STATE_N), (2 * STATE_N) ** -0.5, 0.5, ((1, 8),), jnp.float32),
        "read_im": normal_values(streams_of[10], (LAYERS, GROUPS, GROUP_CH, STATE_N), (2 * STATE_N) ** -0.5, 0.5, ((1, 8),), jnp.float32),
        "skip_weight": normal_values(streams_of[11], (LAYERS, GROUPS, GROUP_CH), 1.0, 4.0, ((1, 8),), jnp.float32),
        "w_out": normal_values(streams_of[12], (LAYERS, WIDTH, D), (WIDTH // 4) ** -0.5, 0.25, ((1, 4), (2, 8))),
        "state_re": normal_values(streams_of[13], (LAYERS, SEQS, GROUPS, STATE_N), 1.0, 6.0, ((1, 4), (2, 8)), jnp.float32),
        "state_im": normal_values(streams_of[14], (LAYERS, SEQS, GROUPS, STATE_N), 1.0, 6.0, ((1, 4), (2, 8)), jnp.float32),
    }


EPSILON = 1e-06
HIGH = lax.Precision.HIGHEST

def state_update(inputs, old_re, old_im, decay_rate, frequency, log_step, map_re, map_im, read_re, read_im, skip_weight):
    lam_re = -decay_rate
    lam_im = frequency
    step_size = jnp.exp(log_step)[:, None]
    magnitude = jnp.exp(lam_re * step_size)
    decay_re = magnitude * jnp.cos(lam_im * step_size)
    decay_im = magnitude * jnp.sin(lam_im * step_size)
    modulus = lam_re * lam_re + lam_im * lam_im
    hold_re = ((decay_re - 1.0) * lam_re + decay_im * lam_im) / modulus
    hold_im = (decay_im * lam_re - (decay_re - 1.0) * lam_im) / modulus
    drive_re = hold_re[:, None, :] * map_re - hold_im[:, None, :] * map_im
    drive_im = hold_re[:, None, :] * map_im + hold_im[:, None, :] * map_re
    push_re = jnp.einsum('bgc,gcn->bgn', inputs, drive_re, precision=HIGH)
    push_im = jnp.einsum('bgc,gcn->bgn', inputs, drive_im, precision=HIGH)
    fresh_re = decay_re * old_re - decay_im * old_im + push_re
    fresh_im = decay_re * old_im + decay_im * old_re + push_im
    readout = jnp.einsum('bgn,gcn->bgc', fresh_re, read_re, precision=HIGH) - jnp.einsum('bgn,gcn->bgc', fresh_im, read_im, precision=HIGH) + skip_weight * inputs
    return (readout, fresh_re, fresh_im)

def reference(tokens, norm_gain, w_in, w_gate, decay_rate, frequency, log_step, map_re, map_im, read_re, read_im, skip_weight, w_out, state_re, state_im):
    hidden = tokens
    all_re = []
    all_im = []
    for layer in range(LAYERS):
        floats = hidden.astype(jnp.float32)
        inv_scale = lax.rsqrt(lax.optimization_barrier(jnp.mean(floats * floats, axis=-1, keepdims=True)) + EPSILON)
        normed = (floats * inv_scale * norm_gain[layer]).astype(jnp.bfloat16)
        projected = jnp.dot(normed, w_in[layer], preferred_element_type=jnp.float32).astype(jnp.bfloat16)
        gate = jnp.dot(normed, w_gate[layer], preferred_element_type=jnp.float32).astype(jnp.bfloat16)
        rows = projected.shape[0]
        inputs = projected.astype(jnp.float32).reshape(rows, GROUPS, GROUP_CH)
        readout, fresh_re, fresh_im = state_update(inputs, state_re[layer], state_im[layer], decay_rate[layer], frequency[layer], log_step[layer], map_re[layer], map_im[layer], read_re[layer], read_im[layer], skip_weight[layer])
        activated = jax.nn.gelu(readout.reshape(rows, WIDTH))
        mixer = (activated * jax.nn.sigmoid(gate.astype(jnp.float32))).astype(jnp.bfloat16)
        mixed = jnp.dot(mixer, w_out[layer], preferred_element_type=jnp.float32)
        hidden = (floats + mixed).astype(jnp.bfloat16)
        all_re.append(fresh_re)
        all_im.append(fresh_im)
    return (hidden, jnp.stack(all_re), jnp.stack(all_im))
```

```python
import functools

import jax
import jax.numpy as jnp
from jax import lax
from jax.experimental import pallas as pl
from jax.experimental.pallas import tpu as pltpu
from jax.sharding import PartitionSpec as P

EPSILON = 1e-06
F32 = jnp.float32
BF16 = jnp.bfloat16
TAIL = 128


def dot(a, b):
    return jnp.dot(a, b, preferred_element_type=F32)


def dot_t(a, b):
    return lax.dot_general(a, b, (((1,), (1,)), ((), ())), preferred_element_type=F32)


def kernel(
    tp_size,
    dp_size,
    bundle,
    tokens,
    gain,
    w_in,
    w_gate,
    rate,
    freq,
    log_step,
    map_re,
    map_im,
    read_re,
    read_im,
    skip,
    w_out,
    state_re,
    state_im,
    hidden_out,
    new_re,
    new_im,
    tok,
    gain_v,
    win_v,
    wgate_v,
    rate_v,
    freq_v,
    step_v,
    mapre_v,
    mapim_v,
    readre_v,
    readim_v,
    skip_v,
    wout_v,
    stre_v,
    stim_v,
    nre_v,
    nim_v,
    drive,
    read,
    held,
    skip_flat,
    xbuf,
    sbuf,
    rbuf,
    mix,
    mbuf,
    obuf,
    orbuf,
    hid,
    load_sem,
    a_send,
    a_recv,
    b_send,
    b_recv,
    c_send,
    c_recv,
    d_send,
    d_recv,
    out_sem,
):
    j = lax.axis_index("tp")
    i = lax.axis_index("dp")
    per = tp_size // dp_size
    layers, groups, states = rate.shape
    channels = skip.shape[2]
    seqs, feats = tokens.shape
    cols = w_in.shape[2]
    depth = w_in.shape[1]
    total_feats = gain.shape[1]
    bundles = groups // bundle
    bc, bn = bundle * channels, bundle * states
    target = lax.div(j, per)
    slot = lax.rem(j, per)
    is_self = target == i

    gain_cols = pl.ds(pl.multiple_of(i * depth, depth), depth)
    loads = [
        (tokens, tok),
        (rate, rate_v),
        (freq, freq_v),
        (log_step, step_v),
        (map_re, mapre_v),
        (map_im, mapim_v),
        (state_re, stre_v),
        (state_im, stim_v),
        (read_re, readre_v),
        (read_im, readim_v),
        (skip, skip_v),
        (gain.at[:, gain_cols], gain_v),
        (w_in, win_v),
        (w_gate, wgate_v),
        (w_out, wout_v),
    ]
    copies = [
        pltpu.make_async_copy(src, dst, load_sem.at[k]) for k, (src, dst) in enumerate(loads)
    ]
    for copy in copies:
        copy.start()

    barrier = pltpu.get_barrier_semaphore()
    for t in range(per):
        for d in range(dp_size):
            src_tp = i * per + t

            @pl.when(jnp.logical_or(src_tp != j, i != d))
            def _():
                pl.semaphore_signal(barrier, inc=1, device_id={"tp": src_tp, "dp": jnp.int32(d)})

    for r in range(1, dp_size):
        pl.semaphore_signal(
            barrier, inc=1, device_id={"tp": j, "dp": lax.rem(i + r, dp_size)}
        )

    pending = []
    order = sorted(range(tp_size), key=lambda r: -min(r, tp_size - r))

    def spread(src, buf, send, recv, layer):
        dst = buf.at[layer, slot, i]
        for r in order:
            copy = pltpu.make_async_remote_copy(
                src_ref=src,
                dst_ref=dst,
                send_sem=send.at[layer, r],
                recv_sem=recv.at[layer, slot, i],
                device_id={"tp": lax.rem(j + r, tp_size), "dp": target},
            )
            if r:
                copy.start()
                pending.append((False, copy))
            else:
                own = pltpu.make_async_copy(src, dst, recv.at[layer, slot, i])

                @pl.when(is_self)
                def _():
                    own.start()

                @pl.when(jnp.logical_not(is_self))
                def _():
                    copy.start()

                pending.append((True, copy))

    def gather_wait(buf, recv, layer):
        for t in range(per):
            for d in range(dp_size):
                ref = buf.at[layer, t, d]
                pltpu.make_async_copy(ref, ref, recv.at[layer, t, d]).wait()

    def scatter(src, dst, send, recv, layer):
        for r in range(dp_size - 1, 0, -1):
            d = lax.rem(i + r, dp_size)
            copy = pltpu.make_async_remote_copy(
                src_ref=src.at[layer, d],
                dst_ref=dst.at[layer, i],
                send_sem=send.at[layer, r],
                recv_sem=recv.at[layer, i],
                device_id={"tp": j, "dp": d},
            )
            copy.start()
            pending.append((False, copy))

    def collect(src, dst, recv, layer):
        acc = src[layer, i].astype(F32)
        for r in range(1, dp_size):
            d = lax.rem(i + r, dp_size)
            ref = dst.at[layer, d]
            pltpu.make_async_copy(ref, ref, recv.at[layer, d]).wait()
            acc = acc + dst[layer, d].astype(F32)
        return acc

    def prepare(layer):
        lam_re = -rate_v[layer]
        lam_im = freq_v[layer]
        eye = lax.broadcasted_iota(jnp.int32, (groups, groups), 0) == lax.broadcasted_iota(
            jnp.int32, (groups, groups), 1
        )
        log_col = jnp.sum(
            jnp.where(eye, step_v[layer : layer + 1, :], 0.0), axis=1, keepdims=True
        )
        step_size = jnp.exp(log_col)
        magnitude = jnp.exp(lam_re * step_size)
        decay_re = magnitude * jnp.cos(lam_im * step_size)
        decay_im = magnitude * jnp.sin(lam_im * step_size)
        modulus = lam_re * lam_re + lam_im * lam_im
        hold_re = ((decay_re - 1.0) * lam_re + decay_im * lam_im) / modulus
        hold_im = (decay_im * lam_re - (decay_re - 1.0) * lam_im) / modulus
        for g in range(groups):
            q, k = g // bundle, g % bundle
            rows = slice(g * channels, (g + 1) * channels)
            to = slice(k * channels, (k + 1) * channels)
            lanes = slice(k * states, (k + 1) * states)
            lanes_im = slice(bn + k * states, bn + (k + 1) * states)
            hr, hi = hold_re[g : g + 1, :], hold_im[g : g + 1, :]
            mr, mi = mapre_v[layer, rows, :], mapim_v[layer, rows, :]
            drive[layer, q, to, lanes] = (hr * mr - hi * mi).astype(BF16)
            drive[layer, q, to, lanes_im] = (hr * mi + hi * mr).astype(BF16)
            read[layer, q, to, lanes] = readre_v[layer, rows, :].astype(BF16)
            read[layer, q, to, lanes_im] = (-readim_v[layer, rows, :]).astype(BF16)
            where = pl.ds(layer * seqs * groups + g, seqs, stride=groups)
            old_re, old_im = stre_v[where, :], stim_v[where, :]
            dr, di = decay_re[g : g + 1, :], decay_im[g : g + 1, :]
            held[layer, q, :, lanes] = dr * old_re - di * old_im
            held[layer, q, :, lanes_im] = dr * old_im + di * old_re
            skip_flat[layer, 0:1, g * channels : (g + 1) * channels] = skip_v[
                layer, g : g + 1, :
            ]

    drive[...] = jnp.zeros_like(drive)
    read[...] = jnp.zeros_like(read)
    copies[0].wait()
    pl.semaphore_wait(barrier, tp_size - is_self.astype(jnp.int32) + dp_size - 1)
    spread(tok, xbuf, a_send, a_recv, 0)
    for copy in copies[1:11]:
        copy.wait()
    for layer in range(layers):
        prepare(layer)
    for copy in copies[11:]:
        copy.wait()

    out_copies = []
    rows_all = dp_size * seqs
    residual = tok[...].astype(F32)
    for layer in range(layers):
        gather_wait(xbuf, a_recv, layer)
        squares = jnp.zeros((rows_all, 1), F32)
        drive_sum = jnp.zeros((rows_all, cols), F32)
        gate_sum = jnp.zeros((rows_all, cols), F32)
        for t in range(per):
            part = slice(t * feats, (t + 1) * feats)
            x = xbuf[layer, t].reshape(rows_all, feats).astype(F32)
            squares = squares + jnp.sum(x * x, axis=1, keepdims=True)
            scaled = (x * gain_v[layer : layer + 1, part]).astype(BF16)
            drive_sum = drive_sum + dot(scaled, win_v[layer, part, :])
            gate_sum = gate_sum + dot(scaled, wgate_v[layer, part, :])
        high = squares.astype(BF16).astype(F32)
        lane = lax.broadcasted_iota(jnp.int32, (rows_all, TAIL), 1)
        tail = jnp.where(lane < TAIL // 2, high, squares - high).astype(BF16)
        sbuf[layer, :, :, 0:TAIL] = tail.reshape(dp_size, seqs, TAIL)
        sbuf[layer, :, :, TAIL : TAIL + cols] = drive_sum.astype(BF16).reshape(
            dp_size, seqs, cols
        )
        sbuf[layer, :, :, TAIL + cols :] = gate_sum.astype(BF16).reshape(dp_size, seqs, cols)
        scatter(sbuf, rbuf, b_send, b_recv, layer)
        acc = collect(sbuf, rbuf, b_recv, layer)
        mean = (acc[:, 0:1] + acc[:, TAIL // 2 : TAIL // 2 + 1]) * (1.0 / total_feats)
        inv_scale = lax.rsqrt(mean + EPSILON)
        projected = (acc[:, TAIL : TAIL + cols] * inv_scale).astype(BF16)
        gate = (acc[:, TAIL + cols :] * inv_scale).astype(BF16).astype(F32)
        fresh = []
        for q in range(bundles):
            part = slice(q * bc, (q + 1) * bc)
            u = projected[:, part]
            new = held[layer, q] + dot(u, drive[layer, q])
            fresh.append(new)
            readout = dot_t(new.astype(BF16), read[layer, q])
            readout = readout + skip_flat[layer, 0:1, part] * u.astype(F32)
            inner = 0.7978845608028654 * (readout + 0.044715 * readout * readout * readout)
            activated = 0.5 * readout * (1.0 + jnp.tanh(inner))
            opened = 0.5 * (jnp.tanh(0.5 * gate[:, part]) + 1.0)
            mix[layer, :, part] = (activated * opened).astype(BF16)
        spread(mix.at[layer], mbuf, c_send, c_recv, layer)
        for g in range(groups):
            q, k = g // bundle, g % bundle
            where = pl.ds(layer * seqs * groups + g, seqs, stride=groups)
            nre_v[where, :] = fresh[q][:, k * states : (k + 1) * states]
            nim_v[where, :] = fresh[q][:, bn + k * states : bn + (k + 1) * states]
        block = pl.ds(layer * seqs * groups, seqs * groups)
        for k, (src, dst) in enumerate(((nre_v, new_re), (nim_v, new_im))):
            copy = pltpu.make_async_copy(src.at[block], dst.at[block], out_sem.at[layer, k])
            copy.start()
            out_copies.append(copy)
        gather_wait(mbuf, c_recv, layer)
        mixed = jnp.zeros((rows_all, feats), F32)
        for t in range(per):
            part = slice(t * cols, (t + 1) * cols)
            mixed = mixed + dot(mbuf[layer, t].reshape(rows_all, cols), wout_v[layer, part, :])
        obuf[layer] = mixed.astype(BF16).reshape(dp_size, seqs, feats)
        scatter(obuf, orbuf, d_send, d_recv, layer)
        hidden = (residual + collect(obuf, orbuf, d_recv, layer)).astype(BF16)
        if layer + 1 < layers:
            hid[layer] = hidden
            spread(hid.at[layer], xbuf, a_send, a_recv, layer + 1)
            residual = hidden.astype(F32)
        else:
            hidden_out[...] = hidden
    for conditional, copy in pending:
        if conditional:

            @pl.when(jnp.logical_not(is_self))
            def _():
                copy.wait_send()
        else:
            copy.wait_send()
    for copy in out_copies:
        copy.wait()


def local(tp_size, dp_size, *args):
    (tokens, gain, w_in, w_gate, rate, freq, log_step, map_re, map_im, read_re, read_im) = args[:11]
    skip, w_out, state_re, state_im = args[11:]
    layers, groups, channels, states = map_re.shape
    seqs, feats = tokens.shape
    depth, cols = w_in.shape[1:]
    per = tp_size // dp_size
    bundle = min(groups, max(1, 128 // channels))
    bundles = groups // bundle
    bc, bn = bundle * channels, bundle * states
    flat = lambda a: a.reshape(layers, groups * channels, states)
    rows = lambda a: a.reshape(layers * seqs * groups, states)
    width = TAIL + 2 * cols
    vm = pltpu.VMEM
    dma = pltpu.SemaphoreType.DMA
    scratch = [
        vm((seqs, feats), BF16),
        vm((layers, depth), F32),
        vm(w_in.shape, BF16),
        vm(w_gate.shape, BF16),
        vm(rate.shape, F32),
        vm(freq.shape, F32),
        vm(log_step.shape, F32),
        vm((layers, groups * channels, states), F32),
        vm((layers, groups * channels, states), F32),
        vm((layers, groups * channels, states), F32),
        vm((layers, groups * channels, states), F32),
        vm(skip.shape, F32),
        vm(w_out.shape, BF16),
        vm((layers * seqs * groups, states), F32),
        vm((layers * seqs * groups, states), F32),
        vm((layers * seqs * groups, states), F32),
        vm((layers * seqs * groups, states), F32),
        vm((layers, bundles, bc, 2 * bn), BF16),
        vm((layers, bundles, bc, 2 * bn), BF16),
        vm((layers, bundles, seqs, 2 * bn), F32),
        vm((layers, 8, cols), F32),
        vm((layers, per, dp_size, seqs, feats), BF16),
        vm((layers, dp_size, seqs, width), BF16),
        vm((layers, dp_size, seqs, width), BF16),
        vm((layers, seqs, cols), BF16),
        vm((layers, per, dp_size, seqs, cols), BF16),
        vm((layers, dp_size, seqs, feats), BF16),
        vm((layers, dp_size, seqs, feats), BF16),
        vm((layers, seqs, feats), BF16),
        dma((15,)),
        dma((layers, tp_size)),
        dma((layers, per, dp_size)),
        dma((layers, dp_size)),
        dma((layers, dp_size)),
        dma((layers, tp_size)),
        dma((layers, per, dp_size)),
        dma((layers, dp_size)),
        dma((layers, dp_size)),
        dma((layers, 2)),
    ]
    hbm = pl.BlockSpec(memory_space=pl.ANY)
    state = jax.ShapeDtypeStruct((layers * seqs * groups, states), F32)
    hidden, new_re, new_im = pl.pallas_call(
        functools.partial(kernel, tp_size, dp_size, bundle),
        out_shape=(jax.ShapeDtypeStruct((seqs, feats), BF16), state, state),
        in_specs=[hbm] * 15,
        out_specs=(pl.BlockSpec(memory_space=pltpu.VMEM), hbm, hbm),
        scratch_shapes=scratch,
        compiler_params=pltpu.CompilerParams(collective_id=0, has_side_effects=True),
    )(
        tokens,
        gain,
        w_in,
        w_gate,
        rate,
        freq,
        log_step,
        flat(map_re),
        flat(map_im),
        flat(read_re),
        flat(read_im),
        skip,
        w_out,
        rows(state_re),
        rows(state_im),
    )
    return hidden, new_re.reshape(state_re.shape), new_im.reshape(state_im.shape)


def solution(mesh):
    return jax.shard_map(
        functools.partial(local, mesh.shape["tp"], mesh.shape["dp"]),
        mesh=mesh,
        in_specs=(
            P("dp", "tp"),
            P(),
            P(None, "dp", "tp"),
            P(None, "dp", "tp"),
            P(None, "tp", None),
            P(None, "tp", None),
            P(None, "tp"),
            P(None, "tp", None, None),
            P(None, "tp", None, None),
            P(None, "tp", None, None),
            P(None, "tp", None, None),
            P(None, "tp", None),
            P(None, "dp", "tp"),
            P(None, "dp", "tp", None),
            P(None, "dp", "tp", None),
        ),
        out_specs=(P("dp", "tp"), P(None, "dp", "tp", None), P(None, "dp", "tp", None)),
        check_vma=False,
    )
```

```python
import functools

import jax
import jax.numpy as jnp
from jax import lax
from jax.experimental import pallas as pl
from jax.experimental.pallas import tpu as pltpu
from jax.sharding import PartitionSpec as P

EPSILON = 1e-06
F32 = jnp.float32
BF16 = jnp.bfloat16
TAIL = 128


def dot(a, b):
    return jnp.dot(a, b, preferred_element_type=F32)


def dot_t(a, b):
    return lax.dot_general(a, b, (((1,), (1,)), ((), ())), preferred_element_type=F32)


def kernel(
    tp_size,
    dp_size,
    bundle,
    tokens,
    gain,
    w_in,
    w_gate,
    rate,
    freq,
    log_step,
    map_re,
    map_im,
    read_re,
    read_im,
    skip,
    w_out,
    state_re,
    state_im,
    hidden_out,
    new_re,
    new_im,
    tok,
    gain_v,
    win_v,
    wgate_v,
    rate_v,
    freq_v,
    step_v,
    mapre_v,
    mapim_v,
    readre_v,
    readim_v,
    skip_v,
    wout_v,
    stre_v,
    stim_v,
    nre_v,
    nim_v,
    drive,
    read,
    held,
    skip_flat,
    xbuf,
    sbuf,
    rbuf,
    mix,
    mbuf,
    obuf,
    orbuf,
    hid,
    load_sem,
    a_send,
    a_recv,
    b_send,
    b_recv,
    c_send,
    c_recv,
    d_send,
    d_recv,
    out_sem,
):
    j = lax.axis_index("tp")
    i = lax.axis_index("dp")
    per = tp_size // dp_size
    layers, groups, states = rate.shape
    channels = skip.shape[2]
    seqs, feats = tokens.shape
    cols = w_in.shape[2]
    depth = w_in.shape[1]
    total_feats = gain.shape[1]
    bundles = groups // bundle
    bc, bn = bundle * channels, bundle * states
    target = lax.div(j, per)
    slot = lax.rem(j, per)
    is_self = target == i

    barrier = pltpu.get_barrier_semaphore()
    for t in range(per):
        for d in range(dp_size):
            src_tp = i * per + t

            @pl.when(jnp.logical_or(src_tp != j, i != d))
            def _():
                pl.semaphore_signal(barrier, inc=1, device_id={"tp": src_tp, "dp": jnp.int32(d)})

    for r in range(1, dp_size):
        pl.semaphore_signal(
            barrier, inc=1, device_id={"tp": j, "dp": lax.rem(i + r, dp_size)}
        )

    gain_cols = pl.ds(pl.multiple_of(i * depth, depth), depth)
    loads = [
        (tokens, tok),
        (rate, rate_v),
        (freq, freq_v),
        (log_step, step_v),
        (map_re, mapre_v),
        (map_im, mapim_v),
        (state_re, stre_v),
        (state_im, stim_v),
        (read_re, readre_v),
        (read_im, readim_v),
        (skip, skip_v),
        (gain.at[:, gain_cols], gain_v),
        (w_in, win_v),
        (w_gate, wgate_v),
        (w_out, wout_v),
    ]
    copies = [
        pltpu.make_async_copy(src, dst, load_sem.at[k]) for k, (src, dst) in enumerate(loads)
    ]
    for copy in copies:
        copy.start()

    pending = []
    order = list(range(tp_size))

    def spread(src, buf, send, recv, layer):
        dst = buf.at[layer, slot, i]
        for r in order:
            copy = pltpu.make_async_remote_copy(
                src_ref=src,
                dst_ref=dst,
                send_sem=send.at[layer, r],
                recv_sem=recv.at[layer, slot, i],
                device_id={"tp": lax.rem(j + r, tp_size), "dp": target},
            )
            if r:
                copy.start()
                pending.append((False, copy))
            else:
                own = pltpu.make_async_copy(src, dst, recv.at[layer, slot, i])

                @pl.when(is_self)
                def _():
                    own.start()

                @pl.when(jnp.logical_not(is_self))
                def _():
                    copy.start()

                pending.append((True, copy))

    def gather_wait(buf, recv, layer):
        for t in range(per):
            for d in range(dp_size):
                ref = buf.at[layer, t, d]
                pltpu.make_async_copy(ref, ref, recv.at[layer, t, d]).wait()

    def scatter(src, dst, send, recv, layer):
        for r in range(dp_size - 1, 0, -1):
            d = lax.rem(i + r, dp_size)
            copy = pltpu.make_async_remote_copy(
                src_ref=src.at[layer, d],
                dst_ref=dst.at[layer, i],
                send_sem=send.at[layer, r],
                recv_sem=recv.at[layer, i],
                device_id={"tp": j, "dp": d},
            )
            copy.start()
            pending.append((False, copy))

    def collect(src, dst, recv, layer):
        acc = src[layer, i].astype(F32)
        for r in range(1, dp_size):
            d = lax.rem(i + r, dp_size)
            ref = dst.at[layer, d]
            pltpu.make_async_copy(ref, ref, recv.at[layer, d]).wait()
            acc = acc + dst[layer, d].astype(F32)
        return acc

    def prepare(layer):
        lam_re = -rate_v[layer]
        lam_im = freq_v[layer]
        eye = lax.broadcasted_iota(jnp.int32, (groups, groups), 0) == lax.broadcasted_iota(
            jnp.int32, (groups, groups), 1
        )
        log_col = jnp.sum(
            jnp.where(eye, step_v[layer : layer + 1, :], 0.0), axis=1, keepdims=True
        )
        step_size = jnp.exp(log_col)
        magnitude = jnp.exp(lam_re * step_size)
        decay_re = magnitude * jnp.cos(lam_im * step_size)
        decay_im = magnitude * jnp.sin(lam_im * step_size)
        modulus = lam_re * lam_re + lam_im * lam_im
        hold_re = ((decay_re - 1.0) * lam_re + decay_im * lam_im) / modulus
        hold_im = (decay_im * lam_re - (decay_re - 1.0) * lam_im) / modulus
        for g in range(groups):
            q, k = g // bundle, g % bundle
            rows = slice(g * channels, (g + 1) * channels)
            to = slice(k * channels, (k + 1) * channels)
            lanes = slice(k * states, (k + 1) * states)
            lanes_im = slice(bn + k * states, bn + (k + 1) * states)
            hr, hi = hold_re[g : g + 1, :], hold_im[g : g + 1, :]
            mr, mi = mapre_v[layer, rows, :], mapim_v[layer, rows, :]
            drive[layer, q, to, lanes] = (hr * mr - hi * mi).astype(BF16)
            drive[layer, q, to, lanes_im] = (hr * mi + hi * mr).astype(BF16)
            read[layer, q, to, lanes] = readre_v[layer, rows, :].astype(BF16)
            read[layer, q, to, lanes_im] = (-readim_v[layer, rows, :]).astype(BF16)
            where = pl.ds(layer * seqs * groups + g, seqs, stride=groups)
            old_re, old_im = stre_v[where, :], stim_v[where, :]
            dr, di = decay_re[g : g + 1, :], decay_im[g : g + 1, :]
            held[layer, q, :, lanes] = dr * old_re - di * old_im
            held[layer, q, :, lanes_im] = dr * old_im + di * old_re
            skip_flat[layer, 0:1, g * channels : (g + 1) * channels] = skip_v[
                layer, g : g + 1, :
            ]

    drive[...] = jnp.zeros_like(drive)
    read[...] = jnp.zeros_like(read)
    copies[0].wait()
    pl.semaphore_wait(barrier, tp_size - is_self.astype(jnp.int32) + dp_size - 1)
    spread(tok, xbuf, a_send, a_recv, 0)
    for copy in copies[1:11]:
        copy.wait()
    for layer in range(layers):
        prepare(layer)
    for copy in copies[11:]:
        copy.wait()

    out_copies = []
    rows_all = dp_size * seqs
    residual = tok[...].astype(F32)
    for layer in range(layers):
        gather_wait(xbuf, a_recv, layer)
        squares = jnp.zeros((rows_all, 1), F32)
        drive_sum = jnp.zeros((rows_all, cols), F32)
        gate_sum = jnp.zeros((rows_all, cols), F32)
        for t in range(per):
            part = slice(t * feats, (t + 1) * feats)
            x = xbuf[layer, t].reshape(rows_all, feats).astype(F32)
            squares = squares + jnp.sum(x * x, axis=1, keepdims=True)
            scaled = (x * gain_v[layer : layer + 1, part]).astype(BF16)
            drive_sum = drive_sum + dot(scaled, win_v[layer, part, :])
            gate_sum = gate_sum + dot(scaled, wgate_v[layer, part, :])
        high = squares.astype(BF16).astype(F32)
        lane = lax.broadcasted_iota(jnp.int32, (rows_all, TAIL), 1)
        tail = jnp.where(lane < TAIL // 2, high, squares - high).astype(BF16)
        sbuf[layer, :, :, 0:TAIL] = tail.reshape(dp_size, seqs, TAIL)
        sbuf[layer, :, :, TAIL : TAIL + cols] = drive_sum.astype(BF16).reshape(
            dp_size, seqs, cols
        )
        sbuf[layer, :, :, TAIL + cols :] = gate_sum.astype(BF16).reshape(dp_size, seqs, cols)
        scatter(sbuf, rbuf, b_send, b_recv, layer)
        acc = collect(sbuf, rbuf, b_recv, layer)
        mean = (acc[:, 0:1] + acc[:, TAIL // 2 : TAIL // 2 + 1]) * (1.0 / total_feats)
        inv_scale = lax.rsqrt(mean + EPSILON)
        projected = (acc[:, TAIL : TAIL + cols] * inv_scale).astype(BF16)
        gate = (acc[:, TAIL + cols :] * inv_scale).astype(BF16).astype(F32)
        fresh = []
        for q in range(bundles):
            part = slice(q * bc, (q + 1) * bc)
            u = projected[:, part]
            new = held[layer, q] + dot(u, drive[layer, q])
            fresh.append(new)
            readout = dot_t(new.astype(BF16), read[layer, q])
            readout = readout + skip_flat[layer, 0:1, part] * u.astype(F32)
            inner = 0.7978845608028654 * (readout + 0.044715 * readout * readout * readout)
            activated = 0.5 * readout * (1.0 + jnp.tanh(inner))
            opened = 0.5 * (jnp.tanh(0.5 * gate[:, part]) + 1.0)
            mix[layer, :, part] = (activated * opened).astype(BF16)
        spread(mix.at[layer], mbuf, c_send, c_recv, layer)
        for g in range(groups):
            q, k = g // bundle, g % bundle
            where = pl.ds(layer * seqs * groups + g, seqs, stride=groups)
            nre_v[where, :] = fresh[q][:, k * states : (k + 1) * states]
            nim_v[where, :] = fresh[q][:, bn + k * states : bn + (k + 1) * states]
        block = pl.ds(layer * seqs * groups, seqs * groups)
        for k, (src, dst) in enumerate(((nre_v, new_re), (nim_v, new_im))):
            copy = pltpu.make_async_copy(src.at[block], dst.at[block], out_sem.at[layer, k])
            copy.start()
            out_copies.append(copy)
        gather_wait(mbuf, c_recv, layer)
        mixed = jnp.zeros((rows_all, feats), F32)
        for t in range(per):
            part = slice(t * cols, (t + 1) * cols)
            mixed = mixed + dot(mbuf[layer, t].reshape(rows_all, cols), wout_v[layer, part, :])
        obuf[layer] = mixed.astype(BF16).reshape(dp_size, seqs, feats)
        scatter(obuf, orbuf, d_send, d_recv, layer)
        hidden = (residual + collect(obuf, orbuf, d_recv, layer)).astype(BF16)
        if layer + 1 < layers:
            hid[layer] = hidden
            spread(hid.at[layer], xbuf, a_send, a_recv, layer + 1)
            residual = hidden.astype(F32)
        else:
            hidden_out[...] = hidden
    for conditional, copy in pending:
        if conditional:

            @pl.when(jnp.logical_not(is_self))
            def _():
                copy.wait_send()
        else:
            copy.wait_send()
    for copy in out_copies:
        copy.wait()


def finish(*refs):
    n = 3
    ins, outs, bufs, sem_in, sem_out = refs[:n], refs[n : 2 * n], refs[2 * n : 3 * n], refs[-2], refs[-1]
    reads = [pltpu.make_async_copy(a, b, sem_in.at[k]) for k, (a, b) in enumerate(zip(ins, bufs))]
    writes = [pltpu.make_async_copy(a, b, sem_out.at[k]) for k, (a, b) in enumerate(zip(bufs, outs))]
    for copy in reads:
        copy.start()
    for a, b in zip(reads, writes):
        a.wait()
        b.start()
    for copy in writes:
        copy.wait()


def local(tp_size, dp_size, *args):
    (tokens, gain, w_in, w_gate, rate, freq, log_step, map_re, map_im, read_re, read_im) = args[:11]
    skip, w_out, state_re, state_im = args[11:]
    layers, groups, channels, states = map_re.shape
    seqs, feats = tokens.shape
    depth, cols = w_in.shape[1:]
    per = tp_size // dp_size
    bundle = min(groups, max(1, 128 // channels))
    bundles = groups // bundle
    bc, bn = bundle * channels, bundle * states
    flat = lambda a: a.reshape(layers, groups * channels, states)
    rows = lambda a: a.reshape(layers * seqs * groups, states)
    width = TAIL + 2 * cols
    vm = pltpu.VMEM
    dma = pltpu.SemaphoreType.DMA
    scratch = [
        vm((seqs, feats), BF16),
        vm((layers, depth), F32),
        vm(w_in.shape, BF16),
        vm(w_gate.shape, BF16),
        vm(rate.shape, F32),
        vm(freq.shape, F32),
        vm(log_step.shape, F32),
        vm((layers, groups * channels, states), F32),
        vm((layers, groups * channels, states), F32),
        vm((layers, groups * channels, states), F32),
        vm((layers, groups * channels, states), F32),
        vm(skip.shape, F32),
        vm(w_out.shape, BF16),
        vm((layers * seqs * groups, states), F32),
        vm((layers * seqs * groups, states), F32),
        vm((layers * seqs * groups, states), F32),
        vm((layers * seqs * groups, states), F32),
        vm((layers, bundles, bc, 2 * bn), BF16),
        vm((layers, bundles, bc, 2 * bn), BF16),
        vm((layers, bundles, seqs, 2 * bn), F32),
        vm((layers, 8, cols), F32),
        vm((layers, per, dp_size, seqs, feats), BF16),
        vm((layers, dp_size, seqs, width), BF16),
        vm((layers, dp_size, seqs, width), BF16),
        vm((layers, seqs, cols), BF16),
        vm((layers, per, dp_size, seqs, cols), BF16),
        vm((layers, dp_size, seqs, feats), BF16),
        vm((layers, dp_size, seqs, feats), BF16),
        vm((layers, seqs, feats), BF16),
        dma((15,)),
        dma((layers, tp_size)),
        dma((layers, per, dp_size)),
        dma((layers, dp_size)),
        dma((layers, dp_size)),
        dma((layers, tp_size)),
        dma((layers, per, dp_size)),
        dma((layers, dp_size)),
        dma((layers, dp_size)),
        dma((layers, 2)),
    ]
    hbm = pl.BlockSpec(memory_space=pl.ANY)
    state = jax.ShapeDtypeStruct((layers * seqs * groups, states), F32)
    hidden, new_re, new_im = pl.pallas_call(
        functools.partial(kernel, tp_size, dp_size, bundle),
        out_shape=(jax.ShapeDtypeStruct((seqs, feats), BF16), state, state),
        in_specs=[hbm] * 15,
        out_specs=(pl.BlockSpec(memory_space=pltpu.VMEM), hbm, hbm),
        scratch_shapes=scratch,
        compiler_params=pltpu.CompilerParams(collective_id=0, has_side_effects=True),
    )(
        tokens,
        gain,
        w_in,
        w_gate,
        rate,
        freq,
        log_step,
        flat(map_re),
        flat(map_im),
        flat(read_re),
        flat(read_im),
        skip,
        w_out,
        rows(state_re),
        rows(state_im),
    )
    hidden, new_re, new_im = pl.pallas_call(
        finish,
        out_shape=(jax.ShapeDtypeStruct((seqs, feats), BF16), state, state),
        in_specs=[hbm] * 3,
        out_specs=[hbm] * 3,
        scratch_shapes=[vm((seqs, feats), BF16), vm(state.shape, F32), vm(state.shape, F32), dma((3,)), dma((3,))],
    )(hidden, new_re, new_im)
    return hidden, new_re.reshape(state_re.shape), new_im.reshape(state_im.shape)


def solution(mesh):
    return jax.shard_map(
        functools.partial(local, mesh.shape["tp"], mesh.shape["dp"]),
        mesh=mesh,
        in_specs=(
            P("dp", "tp"),
            P(),
            P(None, "dp", "tp"),
            P(None, "dp", "tp"),
            P(None, "tp", None),
            P(None, "tp", None),
            P(None, "tp"),
            P(None, "tp", None, None),
            P(None, "tp", None, None),
            P(None, "tp", None, None),
            P(None, "tp", None, None),
            P(None, "tp", None),
            P(None, "dp", "tp"),
            P(None, "dp", "tp", None),
            P(None, "dp", "tp", None),
        ),
        out_specs=(P("dp", "tp"), P(None, "dp", "tp", None), P(None, "dp", "tp", None)),
        check_vma=False,
    )
```

```python
import functools

import jax
import jax.numpy as jnp
from jax import lax
from jax.experimental import pallas as pl
from jax.experimental.pallas import tpu as pltpu
from jax.sharding import PartitionSpec as P

EPSILON = 1e-06
F32 = jnp.float32
BF16 = jnp.bfloat16
TAIL = 128


def dot(a, b):
    return jnp.dot(a, b, preferred_element_type=F32)


def dot_t(a, b):
    return lax.dot_general(a, b, (((1,), (1,)), ((), ())), preferred_element_type=F32)


def kernel(
    tp_size,
    dp_size,
    bundle,
    tokens,
    gain,
    w_in,
    w_gate,
    rate,
    freq,
    log_step,
    map_re,
    map_im,
    read_re,
    read_im,
    skip,
    w_out,
    state_re,
    state_im,
    hidden_out,
    new_re,
    new_im,
    tok,
    gain_v,
    win_v,
    wgate_v,
    rate_v,
    freq_v,
    step_v,
    mapre_v,
    mapim_v,
    readre_v,
    readim_v,
    skip_v,
    wout_v,
    stre_v,
    stim_v,
    nre_v,
    nim_v,
    drive,
    read,
    held,
    skip_flat,
    xbuf,
    sbuf,
    rbuf,
    mix,
    mbuf,
    obuf,
    orbuf,
    hid,
    sgate,
    rgate,
    load_sem,
    a_send,
    a_recv,
    b_send,
    b_recv,
    c_send,
    c_recv,
    d_send,
    d_recv,
    e_send,
    e_recv,
    out_sem,
):
    j = lax.axis_index("tp")
    i = lax.axis_index("dp")
    per = tp_size // dp_size
    layers, groups, states = rate.shape
    channels = skip.shape[2]
    seqs, feats = tokens.shape
    cols = w_in.shape[2]
    depth = w_in.shape[1]
    total_feats = gain.shape[1]
    bundles = groups // bundle
    bc, bn = bundle * channels, bundle * states
    target = lax.div(j, per)
    slot = lax.rem(j, per)
    is_self = target == i

    barrier = pltpu.get_barrier_semaphore()
    for t in range(per):
        for d in range(dp_size):
            src_tp = i * per + t

            @pl.when(jnp.logical_or(src_tp != j, i != d))
            def _():
                pl.semaphore_signal(barrier, inc=1, device_id={"tp": src_tp, "dp": jnp.int32(d)})

    for r in range(1, dp_size):
        pl.semaphore_signal(
            barrier, inc=1, device_id={"tp": j, "dp": lax.rem(i + r, dp_size)}
        )

    gain_cols = pl.ds(pl.multiple_of(i * depth, depth), depth)
    loads = [
        (tokens, tok),
        (rate, rate_v),
        (freq, freq_v),
        (log_step, step_v),
        (map_re, mapre_v),
        (map_im, mapim_v),
        (state_re, stre_v),
        (state_im, stim_v),
        (read_re, readre_v),
        (read_im, readim_v),
        (skip, skip_v),
        (gain.at[:, gain_cols], gain_v),
        (w_in, win_v),
        (w_gate, wgate_v),
        (w_out, wout_v),
    ]
    copies = [
        pltpu.make_async_copy(src, dst, load_sem.at[k]) for k, (src, dst) in enumerate(loads)
    ]
    for copy in copies:
        copy.start()

    pending = []
    order = list(range(tp_size))[::-1]

    def spread(src, buf, send, recv, layer):
        dst = buf.at[layer, slot, i]
        for r in order:
            copy = pltpu.make_async_remote_copy(
                src_ref=src,
                dst_ref=dst,
                send_sem=send.at[layer, r],
                recv_sem=recv.at[layer, slot, i],
                device_id={"tp": lax.rem(j + r, tp_size), "dp": target},
            )
            if r:
                copy.start()
                pending.append((False, copy))
            else:
                own = pltpu.make_async_copy(src, dst, recv.at[layer, slot, i])

                @pl.when(is_self)
                def _():
                    own.start()

                @pl.when(jnp.logical_not(is_self))
                def _():
                    copy.start()

                pending.append((True, copy))

    def gather_wait(buf, recv, layer):
        for t in range(per):
            for d in range(dp_size):
                ref = buf.at[layer, t, d]
                pltpu.make_async_copy(ref, ref, recv.at[layer, t, d]).wait()

    def scatter(src, dst, send, recv, layer):
        for r in range(dp_size - 1, 0, -1):
            d = lax.rem(i + r, dp_size)
            copy = pltpu.make_async_remote_copy(
                src_ref=src.at[layer, d],
                dst_ref=dst.at[layer, i],
                send_sem=send.at[layer, r],
                recv_sem=recv.at[layer, i],
                device_id={"tp": j, "dp": d},
            )
            copy.start()
            pending.append((False, copy))

    def collect(src, dst, recv, layer):
        acc = src[layer, i].astype(F32)
        for r in range(1, dp_size):
            d = lax.rem(i + r, dp_size)
            ref = dst.at[layer, d]
            pltpu.make_async_copy(ref, ref, recv.at[layer, d]).wait()
            acc = acc + dst[layer, d].astype(F32)
        return acc

    def prepare(layer):
        lam_re = -rate_v[layer]
        lam_im = freq_v[layer]
        eye = lax.broadcasted_iota(jnp.int32, (groups, groups), 0) == lax.broadcasted_iota(
            jnp.int32, (groups, groups), 1
        )
        log_col = jnp.sum(
            jnp.where(eye, step_v[layer : layer + 1, :], 0.0), axis=1, keepdims=True
        )
        step_size = jnp.exp(log_col)
        magnitude = jnp.exp(lam_re * step_size)
        decay_re = magnitude * jnp.cos(lam_im * step_size)
        decay_im = magnitude * jnp.sin(lam_im * step_size)
        modulus = lam_re * lam_re + lam_im * lam_im
        hold_re = ((decay_re - 1.0) * lam_re + decay_im * lam_im) / modulus
        hold_im = (decay_im * lam_re - (decay_re - 1.0) * lam_im) / modulus
        for g in range(groups):
            q, k = g // bundle, g % bundle
            rows = slice(g * channels, (g + 1) * channels)
            to = slice(k * channels, (k + 1) * channels)
            lanes = slice(k * states, (k + 1) * states)
            lanes_im = slice(bn + k * states, bn + (k + 1) * states)
            hr, hi = hold_re[g : g + 1, :], hold_im[g : g + 1, :]
            mr, mi = mapre_v[layer, rows, :], mapim_v[layer, rows, :]
            drive[layer, q, to, lanes] = (hr * mr - hi * mi).astype(BF16)
            drive[layer, q, to, lanes_im] = (hr * mi + hi * mr).astype(BF16)
            read[layer, q, to, lanes] = readre_v[layer, rows, :].astype(BF16)
            read[layer, q, to, lanes_im] = (-readim_v[layer, rows, :]).astype(BF16)
            where = pl.ds(layer * seqs * groups + g, seqs, stride=groups)
            old_re, old_im = stre_v[where, :], stim_v[where, :]
            dr, di = decay_re[g : g + 1, :], decay_im[g : g + 1, :]
            held[layer, q, :, lanes] = dr * old_re - di * old_im
            held[layer, q, :, lanes_im] = dr * old_im + di * old_re
            skip_flat[layer, 0:1, g * channels : (g + 1) * channels] = skip_v[
                layer, g : g + 1, :
            ]

    drive[...] = jnp.zeros_like(drive)
    read[...] = jnp.zeros_like(read)
    copies[0].wait()
    pl.semaphore_wait(barrier, tp_size - is_self.astype(jnp.int32) + dp_size - 1)
    spread(tok, xbuf, a_send, a_recv, 0)
    for copy in copies[1:11]:
        copy.wait()
    for layer in range(layers):
        prepare(layer)
    for copy in copies[11:]:
        copy.wait()

    out_copies = []
    rows_all = dp_size * seqs
    residual = tok[...].astype(F32)
    for layer in range(layers):
        gather_wait(xbuf, a_recv, layer)
        squares = jnp.zeros((rows_all, 1), F32)
        drive_sum = jnp.zeros((rows_all, cols), F32)
        operands = []
        for t in range(per):
            part = slice(t * feats, (t + 1) * feats)
            x = xbuf[layer, t].reshape(rows_all, feats).astype(F32)
            squares = squares + jnp.sum(x * x, axis=1, keepdims=True)
            scaled = (x * gain_v[layer : layer + 1, part]).astype(BF16)
            drive_sum = drive_sum + dot(scaled, win_v[layer, part, :])
            operands.append(scaled)
        high = squares.astype(BF16).astype(F32)
        lane = lax.broadcasted_iota(jnp.int32, (rows_all, TAIL), 1)
        tail = jnp.where(lane < TAIL // 2, high, squares - high).astype(BF16)
        sbuf[layer, :, :, 0:TAIL] = tail.reshape(dp_size, seqs, TAIL)
        sbuf[layer, :, :, TAIL:] = drive_sum.astype(BF16).reshape(
            dp_size, seqs, cols
        )
        scatter(sbuf, rbuf, b_send, b_recv, layer)
        gate_sum = jnp.zeros((rows_all, cols), F32)
        for t in range(per):
            part = slice(t * feats, (t + 1) * feats)
            gate_sum = gate_sum + dot(operands[t], wgate_v[layer, part, :])
        sgate[layer] = gate_sum.astype(BF16).reshape(dp_size, seqs, cols)
        scatter(sgate, rgate, e_send, e_recv, layer)
        acc = collect(sbuf, rbuf, b_recv, layer)
        mean = (acc[:, 0:1] + acc[:, TAIL // 2 : TAIL // 2 + 1]) * (1.0 / total_feats)
        inv_scale = lax.rsqrt(mean + EPSILON)
        projected = (acc[:, TAIL:] * inv_scale).astype(BF16)
        fresh, lit = [], []
        for q in range(bundles):
            part = slice(q * bc, (q + 1) * bc)
            u = projected[:, part]
            new = held[layer, q] + dot(u, drive[layer, q])
            fresh.append(new)
            readout = dot_t(new.astype(BF16), read[layer, q])
            readout = readout + skip_flat[layer, 0:1, part] * u.astype(F32)
            inner = 0.7978845608028654 * (readout + 0.044715 * readout * readout * readout)
            lit.append(0.5 * readout * (1.0 + jnp.tanh(inner)))
        gate = collect(sgate, rgate, e_recv, layer) * inv_scale
        gate = gate.astype(BF16).astype(F32)
        for q in range(bundles):
            part = slice(q * bc, (q + 1) * bc)
            opened = 0.5 * (jnp.tanh(0.5 * gate[:, part]) + 1.0)
            mix[layer, :, part] = (lit[q] * opened).astype(BF16)
        spread(mix.at[layer], mbuf, c_send, c_recv, layer)
        for g in range(groups):
            q, k = g // bundle, g % bundle
            where = pl.ds(layer * seqs * groups + g, seqs, stride=groups)
            nre_v[where, :] = fresh[q][:, k * states : (k + 1) * states]
            nim_v[where, :] = fresh[q][:, bn + k * states : bn + (k + 1) * states]
        block = pl.ds(layer * seqs * groups, seqs * groups)
        for k, (src, dst) in enumerate(((nre_v, new_re), (nim_v, new_im))):
            copy = pltpu.make_async_copy(src.at[block], dst.at[block], out_sem.at[layer, k])
            copy.start()
            out_copies.append(copy)
        gather_wait(mbuf, c_recv, layer)
        mixed = jnp.zeros((rows_all, feats), F32)
        for t in range(per):
            part = slice(t * cols, (t + 1) * cols)
            mixed = mixed + dot(mbuf[layer, t].reshape(rows_all, cols), wout_v[layer, part, :])
        obuf[layer] = mixed.astype(BF16).reshape(dp_size, seqs, feats)
        scatter(obuf, orbuf, d_send, d_recv, layer)
        hidden = (residual + collect(obuf, orbuf, d_recv, layer)).astype(BF16)
        if layer + 1 < layers:
            hid[layer] = hidden
            spread(hid.at[layer], xbuf, a_send, a_recv, layer + 1)
            residual = hidden.astype(F32)
        else:
            hidden_out[...] = hidden
    for conditional, copy in pending:
        if conditional:

            @pl.when(jnp.logical_not(is_self))
            def _():
                copy.wait_send()
        else:
            copy.wait_send()
    for copy in out_copies:
        copy.wait()


def finish(*refs):
    n = 3
    ins, outs, bufs, sem_in, sem_out = refs[:n], refs[n : 2 * n], refs[2 * n : 3 * n], refs[-2], refs[-1]
    reads = [pltpu.make_async_copy(a, b, sem_in.at[k]) for k, (a, b) in enumerate(zip(ins, bufs))]
    writes = [pltpu.make_async_copy(a, b, sem_out.at[k]) for k, (a, b) in enumerate(zip(bufs, outs))]
    for copy in reads:
        copy.start()
    for a, b in zip(reads, writes):
        a.wait()
        b.start()
    for copy in writes:
        copy.wait()


def local(tp_size, dp_size, *args):
    (tokens, gain, w_in, w_gate, rate, freq, log_step, map_re, map_im, read_re, read_im) = args[:11]
    skip, w_out, state_re, state_im = args[11:]
    layers, groups, channels, states = map_re.shape
    seqs, feats = tokens.shape
    depth, cols = w_in.shape[1:]
    per = tp_size // dp_size
    bundle = min(groups, max(1, 128 // channels))
    bundles = groups // bundle
    bc, bn = bundle * channels, bundle * states
    flat = lambda a: a.reshape(layers, groups * channels, states)
    rows = lambda a: a.reshape(layers * seqs * groups, states)
    width = TAIL + cols
    vm = pltpu.VMEM
    dma = pltpu.SemaphoreType.DMA
    scratch = [
        vm((seqs, feats), BF16),
        vm((layers, depth), F32),
        vm(w_in.shape, BF16),
        vm(w_gate.shape, BF16),
        vm(rate.shape, F32),
        vm(freq.shape, F32),
        vm(log_step.shape, F32),
        vm((layers, groups * channels, states), F32),
        vm((layers, groups * channels, states), F32),
        vm((layers, groups * channels, states), F32),
        vm((layers, groups * channels, states), F32),
        vm(skip.shape, F32),
        vm(w_out.shape, BF16),
        vm((layers * seqs * groups, states), F32),
        vm((layers * seqs * groups, states), F32),
        vm((layers * seqs * groups, states), F32),
        vm((layers * seqs * groups, states), F32),
        vm((layers, bundles, bc, 2 * bn), BF16),
        vm((layers, bundles, bc, 2 * bn), BF16),
        vm((layers, bundles, seqs, 2 * bn), F32),
        vm((layers, 8, cols), F32),
        vm((layers, per, dp_size, seqs, feats), BF16),
        vm((layers, dp_size, seqs, width), BF16),
        vm((layers, dp_size, seqs, width), BF16),
        vm((layers, seqs, cols), BF16),
        vm((layers, per, dp_size, seqs, cols), BF16),
        vm((layers, dp_size, seqs, feats), BF16),
        vm((layers, dp_size, seqs, feats), BF16),
        vm((layers, seqs, feats), BF16),
        vm((layers, dp_size, seqs, cols), BF16),
        vm((layers, dp_size, seqs, cols), BF16),
        dma((15,)),
        dma((layers, tp_size)),
        dma((layers, per, dp_size)),
        dma((layers, dp_size)),
        dma((layers, dp_size)),
        dma((layers, tp_size)),
        dma((layers, per, dp_size)),
        dma((layers, dp_size)),
        dma((layers, dp_size)),
        dma((layers, dp_size)),
        dma((layers, dp_size)),
        dma((layers, 2)),
    ]
    hbm = pl.BlockSpec(memory_space=pl.ANY)
    state = jax.ShapeDtypeStruct((layers * seqs * groups, states), F32)
    hidden, new_re, new_im = pl.pallas_call(
        functools.partial(kernel, tp_size, dp_size, bundle),
        out_shape=(jax.ShapeDtypeStruct((seqs, feats), BF16), state, state),
        in_specs=[hbm] * 15,
        out_specs=(pl.BlockSpec(memory_space=pltpu.VMEM), hbm, hbm),
        scratch_shapes=scratch,
        compiler_params=pltpu.CompilerParams(collective_id=0, has_side_effects=True),
    )(
        tokens,
        gain,
        w_in,
        w_gate,
        rate,
        freq,
        log_step,
        flat(map_re),
        flat(map_im),
        flat(read_re),
        flat(read_im),
        skip,
        w_out,
        rows(state_re),
        rows(state_im),
    )
    hidden, new_re, new_im = pl.pallas_call(
        finish,
        out_shape=(jax.ShapeDtypeStruct((seqs, feats), BF16), state, state),
        in_specs=[hbm] * 3,
        out_specs=[hbm] * 3,
        scratch_shapes=[vm((seqs, feats), BF16), vm(state.shape, F32), vm(state.shape, F32), dma((3,)), dma((3,))],
    )(hidden, new_re, new_im)
    return hidden, new_re.reshape(state_re.shape), new_im.reshape(state_im.shape)


def solution(mesh):
    return jax.shard_map(
        functools.partial(local, mesh.shape["tp"], mesh.shape["dp"]),
        mesh=mesh,
        in_specs=(
            P("dp", "tp"),
            P(),
            P(None, "dp", "tp"),
            P(None, "dp", "tp"),
            P(None, "tp", None),
            P(None, "tp", None),
            P(None, "tp"),
            P(None, "tp", None, None),
            P(None, "tp", None, None),
            P(None, "tp", None, None),
            P(None, "tp", None, None),
            P(None, "tp", None),
            P(None, "dp", "tp"),
            P(None, "dp", "tp", None),
            P(None, "dp", "tp", None),
        ),
        out_specs=(P("dp", "tp"), P(None, "dp", "tp", None), P(None, "dp", "tp", None)),
        check_vma=False,
    )
```
